32 devices in a mesh: ep: 8 (over z, x), tp: 4 (over y, core).
Axes of the slice: x: 2, y: 2, z: 4, core: 2. Of those that a mesh axis runs over, the one named last changes fastest.
Arguments:
- tokens: bfloat16 [128, 4096], P('ep'), may hold values from -6 to 6
- norm_gain: float32 [4096], replicated, may hold values from 0.1 to 1.9
- query_weight: bfloat16 [4096, 2048], P('ep', 'tp'), may hold values from -0.09375 to 0.09375
- key_weight: bfloat16 [4096, 256], P('ep', 'tp'), may hold values from -0.09375 to 0.09375
- value_weight: bfloat16 [4096, 256], P('ep', 'tp'), may hold values from -0.09375 to 0.09375
- forget_weight: bfloat16 [4096, 32], P('ep', 'tp'), may hold values from -0.09375 to 0.09375
- forget_bias: float32 [32], P('tp'), may hold values from -1 to 2
- kv_cache: bfloat16 [128, 1024, 4, 128], P('ep', None, 'tp'), may hold values from -256 to 256, as said below
- log_gates: float32 [128, 1024, 32], P('ep', None, 'tp'), may hold values from -258 to 0
- lengths: int32 [128], P('ep'), may hold values from 128 to 1024, as said below
- out_weight: bfloat16 [2048, 4096], P('tp', 'ep'), may hold values from -0.125 to 0.125
- mix_gain: float32 [4096], replicated, may hold values from 0.1 to 1.9
- expert_gate: bfloat16 [8, 4096, 1024], P('ep', None, 'tp'), may hold values from -0.09375 to 0.09375
- expert_up: bfloat16 [8, 4096, 1024], P('ep', None, 'tp'), may hold values from -0.09375 to 0.09375
- expert_down: bfloat16 [8, 1024, 4096], P('ep', 'tp'), may hold values from -0.1875 to 0.1875
- routes: int32 [128, 4], P('ep'), may hold values from 0 to 7, all different within a row; in each aligned block of 16 rows (0 to 15, 16 to 31, ...) at most 16 rows name the same one
- route_weights: float32 [128, 4], P('ep'), may hold values from 0.2 to 1
- dense_gate: bfloat16 [4096, 4096], P(None, 'ep'), may hold values from -0.09375 to 0.09375
- dense_up: bfloat16 [4096, 4096], P(None, 'ep'), may hold values from -0.09375 to 0.09375
- dense_down: bfloat16 [4096, 4096], P('ep', 'tp'), may hold values from -0.09375 to 0.09375
- gate_vector: float32 [4096], replicated, may hold values from -0.09375 to 0.09375
Outputs:
- layer_out: bfloat16 [128, 4096], P('ep', 'tp')
The draws below stay inside these ranges and needn't reach their ends.
Inputs may be any that keep to these rules, and one draw needn't show every extreme that they name: `kv_cache`: keys and values of the cached positions. `lengths`: some sequence uses all 1024 cached positions in every draw. A sequence's 4 experts differ. Among the routes of the 16 sequences of one index of ep no expert appears more than 16 times, and in every draw some expert appears exactly 16 times there; every expert is chosen somewhere.
All inputs are finite; a program needn't handle non-finite values.
Results may differ from the reference program's by a relative error of at most 0.012.
The reference program's roundings to bfloat16 on the way count: a program that leaves them out, or rounds other values in their place, can miss the bound.
Values may be sent and summed in bfloat16 or wider, within the bound.
No kernel may reach another device: no remote copies, remote signals or barrier semaphores. Data moves between devices by JAX's collectives and lax.ppermute only.
A program may use at most 128 MiB of HBM per device.

```python
import math
import jax
import jax.numpy as jnp
import numpy as np
from jax import lax

D = 4096
HEADS = 32
KV_HEADS = 4
HD = 64
FE = 1024
FS = 4096
TOPK = 4
SEQ_DEV = 16
CACHE_POSITIONS = 1024
SEQUENCE_TOTAL = 128
EXPERTS = 8
CAP = 16
N_EP = 8


def log_uniform(stream, shape, low, high):
    return jnp.exp(jax.random.uniform(stream, shape, jnp.float32, math.log(low), math.log(high)))


def draw_kv_cache(key, part):
    sequence_flows = jax.random.split(key, 2)
    key_shape = (SEQUENCE_TOTAL, CACHE_POSITIONS, KV_HEADS, HD)
    key_part = jnp.clip(jax.random.normal(sequence_flows[0], key_shape, jnp.float32), -6.0, 6.0)
    value_base = jnp.clip(jax.random.normal(sequence_flows[1], key_shape, jnp.float32), -6.0, 6.0)
    return jnp.concatenate([key_part, value_base], axis=-1).astype(jnp.bfloat16)


def draw_log_gates(key, part):
    sequence_flows = jax.random.split(key, 8)
    slow_share = 0.5
    slow = jax.random.uniform(sequence_flows[0], (HEADS,)) < slow_share
    slow_total = log_uniform(sequence_flows[1], (HEADS,), 0.1, 0.5)
    fast_rate = log_uniform(sequence_flows[2], (HEADS,), 1.0 / 100.0, 1.0 / 30.0)
    base_rate = jnp.where(slow, slow_total / CACHE_POSITIONS, fast_rate)
    seq_factor = log_uniform(sequence_flows[3], (SEQUENCE_TOTAL, 1, 1), 0.5, 2.0)
    block_factor = jnp.repeat(log_uniform(sequence_flows[4], (SEQUENCE_TOTAL, 16, 1), 0.5, 2.0), CACHE_POSITIONS // 16, axis=1)
    roughness = jax.random.uniform(sequence_flows[5], (SEQUENCE_TOTAL, CACHE_POSITIONS, HEADS), jnp.float32, 0.5, 1.5)
    spike_locations = jax.random.randint(sequence_flows[6], (SEQUENCE_TOTAL, 2), 0, CACHE_POSITIONS)
    current_position = jnp.arange(CACHE_POSITIONS)
    spiking = jnp.any(current_position[None, :, None] == spike_locations[:, None, :], axis=2)
    spike_length = jax.random.uniform(sequence_flows[7], (SEQUENCE_TOTAL, CACHE_POSITIONS, 1), jnp.float32, 0.22, 0.5)
    reduction_amount = base_rate[None, None, :] * seq_factor * block_factor * roughness
    reduction_amount = reduction_amount + jnp.where(spiking[:, :, None], spike_length, 0.0)
    return jnp.cumsum(-reduction_amount, axis=1)


def draw_lengths(key, part):
    sequence_flows = jax.random.split(key, 2)
    picked = jax.random.randint(sequence_flows[0], (SEQUENCE_TOTAL,), CACHE_POSITIONS // 8, CACHE_POSITIONS + 1)
    chosen = jax.random.randint(sequence_flows[1], (), 0, SEQUENCE_TOTAL)
    return jnp.where(jnp.arange(SEQUENCE_TOTAL) == chosen, CACHE_POSITIONS, picked).astype(jnp.int32)


def steps_of(rng, dims, cuts, smallest, high):
    loudness = 1.0
    for position, blocks in cuts:
        steps = jax.random.uniform(jax.random.fold_in(jax.random.fold_in(rng, 6), position), (blocks,), jnp.float32, smallest / len(cuts), high / len(cuts))
        loudness = loudness * jnp.repeat(jnp.exp(steps), dims[position] // blocks).reshape((-1,) + (1,) * (len(dims) - 1 - position))
    return loudness


def assign_block(rng, own, number, rows, count, top, most, skew):
    ranking = jax.random.permutation(rng, count)
    packed, ordinary = portions_of(count, rows * top, most, skew, True), portions_of(count, rows * top, most, skew, False)
    places = jnp.arange(count)

    def named(tallies, offset_by):
        used = int((tallies > 0).sum())
        fixed = max(1, used // 4)
        moved = fixed + (places - fixed + offset_by * (used - fixed)) % max(1, count - fixed)
        return jnp.zeros((count,), jnp.int32).at[ranking[jnp.where(places < fixed, places, moved)]].set(jnp.asarray(tallies, jnp.int32))

    tallies = jnp.where(number % 4 == 0, named(packed, number // 4), named(ordinary, number - number // 4 - 1))
    mixed = jax.random.permutation(jax.random.fold_in(own, 3), count)
    giver, taker = mixed[0:count // 2 * 2:2], mixed[1:count // 2 * 2:2]
    margin = jnp.minimum(tallies[giver] - 1, most - tallies[taker]) // 2
    margin = jnp.where((giver == ranking[0]) | (taker == ranking[0]) | (tallies[taker] == 0), 0, jnp.maximum(margin, 0))
    moved = jax.random.randint(jax.random.fold_in(own, 4), (count // 2,), 0, 1 << 20) % (margin + 1)
    tallies = tallies.at[giver].add(-moved).at[taker].add(moved)
    members = jnp.searchsorted(jnp.cumsum(tallies), jnp.arange(rows * top), side="right").astype(jnp.int32)
    table = members.reshape(top, rows).T
    table = table[jax.random.permutation(jax.random.fold_in(own, 1), rows)]
    offset_by = jax.random.randint(jax.random.fold_in(own, 2), (rows, 1), 0, top)
    return jnp.take_along_axis(table, (jnp.arange(top)[None, :] + offset_by) % top, axis=1)


def portions_of(amount, total, reach, lean, full):
    weights = [(1 << 20) // math.isqrt(grade ** lean) + 1 for grade in range(1, amount + 1)]
    largest = reach if full else min(reach, max(-(-total // amount), total * weights[0] // sum(weights)))
    least = 1 if total - largest >= amount - 1 else 0
    holding, surplus = [largest] + [least] * (amount - 1), total - largest - least * (amount - 1)
    while surplus > 0:
        movable = [i for i in range(1, amount) if holding[i] < largest] or [i for i in range(1, amount) if holding[i] < reach]
        pool, left = sum([weights[i] for i in movable]), surplus
        for i in movable:
            addition = min(reach - holding[i], max(1, left * weights[i] // pool), surplus)
            holding[i] = holding[i] + addition
            surplus = surplus - addition
    return np.array(holding)


def gaussian(stream_key, dims, spread, limit, pieces=(), kind=jnp.bfloat16):
    values = jax.random.normal(stream_key, dims, jnp.float32) * spread
    if len(pieces) > 0:
        values = steps_of(stream_key, dims, pieces, -0.22, 0.18) * values
    return jnp.clip(values, min=-limit, max=limit).astype(kind)


def setup_inputs(seed: int = 0) -> dict:
    arg_keys = jax.random.split(jax.random.key(seed), 22)
    tokens = gaussian(arg_keys[0], (SEQUENCE_TOTAL, D), 1.0, 6.0, ((0, 8),))
    norm_gain = jnp.clip(1.0 + 0.18 * jax.random.normal(arg_keys[1], (D,), jnp.float32), 0.1, 1.9)
    query_weight = gaussian(arg_keys[2], (D, HEADS * HD), D ** -0.5, 0.09375, ((0, 8), (1, 4)))
    key_weight = gaussian(arg_keys[3], (D, KV_HEADS * HD), D ** -0.5, 0.09375, ((0, 8), (1, 4)))
    value_weight = gaussian(arg_keys[4], (D, KV_HEADS * HD), D ** -0.5, 0.09375, ((0, 8), (1, 4)))
    forget_weight = gaussian(arg_keys[5], (D, HEADS), D ** -0.5, 0.09375, ((0, 8), (1, 4)))
    forget_bias = jnp.clip(-1.0 + 3.0 * jax.random.uniform(arg_keys[6], (HEADS,), jnp.float32) ** steps_of(arg_keys[6], (HEADS,), ((0, 4),), -0.2, 0.2), -1.0, 2.0)
    kv_cache = draw_kv_cache(jax.random.fold_in(arg_keys[21], 71), 0)
    log_gates = draw_log_gates(jax.random.fold_in(arg_keys[21], 71), 0)
    lengths = draw_lengths(jax.random.fold_in(arg_keys[21], 71), 0)
    out_weight = gaussian(arg_keys[10], (HEADS * HD, D), (HEADS * HD) ** -0.5, 0.125, ((0, 4), (1, 8)))
    mix_gain = jnp.clip(1.0 + 0.18 * jax.random.normal(arg_keys[11], (D,), jnp.float32), 0.1, 1.9)
    expert_gate = gaussian(arg_keys[12], (EXPERTS, D, FE), D ** -0.5, 0.09375, ((0, 8), (2, 4)))
    expert_up = gaussian(arg_keys[13], (EXPERTS, D, FE), D ** -0.5, 0.09375, ((0, 8), (2, 4)))
    expert_down = gaussian(arg_keys[14], (EXPERTS, FE, D), FE ** -0.5, 0.1875, ((0, 8), (1, 4)))
    routes_keys = jax.random.split(jax.random.fold_in(arg_keys[15], 1), SEQUENCE_TOTAL // SEQ_DEV)
    routes_turns = jax.random.permutation(jax.random.fold_in(arg_keys[15], 3), SEQUENCE_TOTAL // SEQ_DEV)
    routes = jax.vmap(lambda own, number: assign_block(jax.random.fold_in(arg_keys[15], 2), own, number, SEQ_DEV, EXPERTS, TOPK, CAP, 2))(routes_keys, routes_turns).reshape((SEQUENCE_TOTAL, TOPK))
    route_weights = jnp.clip(0.2 + 0.8 * jax.random.uniform(arg_keys[16], (SEQUENCE_TOTAL, TOPK), jnp.float32) ** steps_of(arg_keys[16], (SEQUENCE_TOTAL, TOPK), ((0, 8),), -0.2, 0.2), 0.2, 1.0)
    dense_gate = gaussian(arg_keys[17], (D, FS), D ** -0.5, 0.09375, ((1, 8),))
    dense_up = gaussian(arg_keys[18], (D, FS), D ** -0.5, 0.09375, ((1, 8),))
    dense_down = gaussian(arg_keys[19], (FS, D), FS ** -0.5, 0.09375, ((0, 8), (1, 4)))
    gate_vector = gaussian(arg_keys[20], (D,), D ** -0.5, 0.09375, (), jnp.float32)
    return {"tokens": tokens, "norm_gain": norm_gain, "query_weight": query_weight, "key_weight": key_weight, "value_weight": value_weight, "forget_weight": forget_weight, "forget_bias": forget_bias, "kv_cache": kv_cache, "log_gates": log_gates, "lengths": lengths, "out_weight": out_weight, "mix_gain": mix_gain, "expert_gate": expert_gate, "expert_up": expert_up, "expert_down": expert_down, "routes": routes, "route_weights": route_weights, "dense_gate": dense_gate, "dense_up": dense_up, "dense_down": dense_down, "gate_vector": gate_vector}


EPS = 1e-06

def rms_scaled(matrix, gains):
    values = matrix.astype(jnp.float32)
    return values * lax.rsqrt(lax.optimization_barrier(jnp.mean(values * values, axis=-1, keepdims=True)) + EPS) * gains.astype(jnp.float32)

def attend_block(inputs):
    queries, key_new, value_new, forget, cache_rows, cum_gates, length = inputs
    seqs_here, cache_len = (cache_rows.shape[0], cache_rows.shape[1])
    kv_count, group_size, head_width = (queries.shape[1], queries.shape[2], queries.shape[3])
    cached_keys = cache_rows[..., :head_width].astype(jnp.float32)
    cached_values = cache_rows[..., head_width:].astype(jnp.float32)
    query_wide = queries.astype(jnp.float32)
    score_scale = head_width ** (-0.5)
    current_position = jnp.arange(cache_len, dtype=jnp.int32)
    is_last = (current_position[None, :] == length[:, None] - 1)[:, :, None]
    last_gate = lax.optimization_barrier(jnp.sum(jnp.where(is_last, cum_gates, 0.0), axis=1))
    newest = last_gate + forget
    gate_bias = newest[:, None, :] - cum_gates
    gate_bias = gate_bias.reshape(seqs_here, cache_len, kv_count, group_size).transpose(0, 2, 3, 1)
    past_scores = jnp.einsum('skgd,slkd->skgl', query_wide, cached_keys) * score_scale + gate_bias
    is_valid = (current_position[None, :] < length[:, None])[:, None, None, :]
    past_scores = jnp.where(is_valid, past_scores, -jnp.inf)
    own_score = jnp.einsum('skgd,skd->skg', query_wide, key_new.astype(jnp.float32)) * score_scale
    highest = jnp.maximum(lax.optimization_barrier(jnp.max(past_scores, axis=-1)), own_score)
    past_exp = jnp.exp(past_scores - highest[..., None])
    own_exp = jnp.exp(own_score - highest)
    totals = lax.optimization_barrier(jnp.sum(past_exp, axis=-1)) + own_exp
    past_weights = (past_exp / totals[..., None]).astype(jnp.bfloat16)
    own_weights = (own_exp / totals).astype(jnp.bfloat16)
    mixed_values = jnp.einsum('skgl,slkd->skgd', past_weights.astype(jnp.float32), cached_values)
    mixed_values = mixed_values + own_weights.astype(jnp.float32)[..., None] * value_new.astype(jnp.float32)[:, :, None, :]
    return mixed_values.astype(jnp.bfloat16).reshape(seqs_here, kv_count * group_size * head_width)

def reference(tokens, norm_gain, query_weight, key_weight, value_weight, forget_weight, forget_bias, kv_cache, log_gates, lengths, out_weight, mix_gain, expert_gate, expert_up, expert_down, routes, route_weights, dense_gate, dense_up, dense_down, gate_vector):
    group_size = HEADS // KV_HEADS
    normed = rms_scaled(tokens, norm_gain).astype(jnp.bfloat16)
    queries = jnp.dot(normed, query_weight, preferred_element_type=jnp.float32).astype(jnp.bfloat16)
    key_new = jnp.dot(normed, key_weight, preferred_element_type=jnp.float32).astype(jnp.bfloat16)
    value_new = jnp.dot(normed, value_weight, preferred_element_type=jnp.float32).astype(jnp.bfloat16)
    forget = jax.nn.log_sigmoid(jnp.dot(normed, forget_weight, preferred_element_type=jnp.float32) + forget_bias)
    blocks = (queries.reshape(N_EP, SEQ_DEV, KV_HEADS, group_size, HD), key_new.reshape(N_EP, SEQ_DEV, KV_HEADS, HD), value_new.reshape(N_EP, SEQ_DEV, KV_HEADS, HD), forget.reshape(N_EP, SEQ_DEV, HEADS), kv_cache.reshape(N_EP, SEQ_DEV, CACHE_POSITIONS, KV_HEADS, 2 * HD), log_gates.reshape(N_EP, SEQ_DEV, CACHE_POSITIONS, HEADS), lengths.reshape(N_EP, SEQ_DEV))
    attended = lax.map(attend_block, blocks).reshape(SEQUENCE_TOTAL, HEADS * HD)
    mixed = (tokens.astype(jnp.float32) + jnp.dot(attended, out_weight, preferred_element_type=jnp.float32)).astype(jnp.bfloat16)
    second = rms_scaled(mixed, mix_gain).astype(jnp.bfloat16)
    gate_value = jax.nn.sigmoid(jnp.dot(second.astype(jnp.float32), gate_vector, precision=lax.Precision.HIGHEST))
    dense_hidden = (jax.nn.silu(jnp.dot(second, dense_gate, preferred_element_type=jnp.float32)) * jnp.dot(second, dense_up, preferred_element_type=jnp.float32)).astype(jnp.bfloat16)
    dense_out = jnp.dot(dense_hidden, dense_down, preferred_element_type=jnp.float32)
    most_rows = N_EP * CAP
    flat_routes = routes.reshape(-1)
    flat_weights = route_weights.reshape(-1)
    token_rows = jnp.arange(SEQUENCE_TOTAL * TOPK, dtype=jnp.int32) // TOPK

    def one_expert(routed, inputs):
        expert_index, gate_matrix, up_matrix, down_matrix = inputs
        is_mine = flat_routes == expert_index
        row_order = jnp.argsort(jnp.where(is_mine, 0, 1).astype(jnp.int32), stable=True)[:most_rows]
        chosen_tokens = token_rows[row_order]
        chosen_weights = jnp.where(is_mine[row_order], flat_weights[row_order], 0.0)
        picked = second[chosen_tokens]
        hidden = (jax.nn.silu(jnp.dot(picked, gate_matrix, preferred_element_type=jnp.float32)) * jnp.dot(picked, up_matrix, preferred_element_type=jnp.float32)).astype(jnp.bfloat16)
        result = jnp.dot(hidden, down_matrix, preferred_element_type=jnp.float32).astype(jnp.bfloat16)
        result = lax.optimization_barrier(result).astype(jnp.float32)
        return (routed.at[chosen_tokens].add(chosen_weights[:, None] * result), None)
    routed = lax.scan(one_expert, jnp.zeros((SEQUENCE_TOTAL, D), jnp.float32), (jnp.arange(EXPERTS, dtype=jnp.int32), expert_gate, expert_up, expert_down))[0]
    return (mixed.astype(jnp.float32) + routed + gate_value[:, None] * dense_out).astype(jnp.bfloat16)
```

```python
import jax
import jax.numpy as jnp
from jax import lax
from jax.experimental import pallas as pl
from jax.experimental.pallas import tpu as pltpu
from jax.sharding import PartitionSpec as P

EPS = 1e-06


def rms_scaled(matrix, gains):
    values = matrix.astype(jnp.float32)
    return values * lax.rsqrt(jnp.mean(values * values, axis=-1, keepdims=True) + EPS) * gains


def attend_local(queries, key_new, value_new, forget, kv_cache, log_gates, lengths):
    seqs_here, cache_len, kv_count, double_width = kv_cache.shape
    head_width = double_width // 2
    group_size = queries.shape[1] // (kv_count * head_width)
    queries = queries.reshape(seqs_here, kv_count, group_size, head_width)
    key_new = key_new.reshape(seqs_here, kv_count, head_width)
    value_new = value_new.reshape(seqs_here, kv_count, head_width)
    cached_keys = kv_cache[..., :head_width]
    cached_values = kv_cache[..., head_width:]
    score_scale = head_width ** (-0.5)
    current_position = jnp.arange(cache_len, dtype=jnp.int32)
    is_last = (current_position[None, :] == lengths[:, None] - 1)[:, :, None]
    last_gate = jnp.sum(jnp.where(is_last, log_gates, 0.0), axis=1)
    newest = last_gate + forget
    gate_bias = newest[:, None, :] - log_gates
    gate_bias = gate_bias.reshape(seqs_here, cache_len, kv_count, group_size).transpose(0, 2, 3, 1)
    past_scores = (
        jnp.einsum("skgd,slkd->skgl", queries, cached_keys, preferred_element_type=jnp.float32)
        * score_scale
        + gate_bias
    )
    is_valid = (current_position[None, :] < lengths[:, None])[:, None, None, :]
    past_scores = jnp.where(is_valid, past_scores, -jnp.inf)
    own_score = (
        jnp.einsum("skgd,skd->skg", queries, key_new, preferred_element_type=jnp.float32)
        * score_scale
    )
    highest = jnp.maximum(jnp.max(past_scores, axis=-1), own_score)
    past_exp = jnp.exp(past_scores - highest[..., None])
    own_exp = jnp.exp(own_score - highest)
    totals = jnp.sum(past_exp, axis=-1) + own_exp
    past_weights = (past_exp / totals[..., None]).astype(jnp.bfloat16)
    own_weights = (own_exp / totals).astype(jnp.bfloat16)
    mixed_values = jnp.einsum(
        "skgl,slkd->skgd", past_weights, cached_values, preferred_element_type=jnp.float32
    )
    mixed_values = (
        mixed_values
        + own_weights.astype(jnp.float32)[..., None] * value_new.astype(jnp.float32)[:, :, None, :]
    )
    return mixed_values.astype(jnp.bfloat16).reshape(seqs_here, kv_count * group_size * head_width)


def swap_bit(value, axis, bit):
    count = lax.axis_size(axis)
    return lax.ppermute(value, axis, [(i, i ^ bit) for i in range(count)])


def bits_of(axis):
    count = lax.axis_size(axis)
    return [1 << k for k in range(count.bit_length() - 1)]


def keep_block(blocks, axis):
    index = lax.axis_index(axis)
    for bit in bits_of(axis):
        count = blocks.shape[0]
        pairs = blocks.reshape((count // 2, 2) + blocks.shape[1:])
        high = (index & bit) > 0
        sent = jnp.where(high, pairs[:, 0], pairs[:, 1]).astype(jnp.bfloat16)
        kept = jnp.where(high, pairs[:, 1], pairs[:, 0]).astype(jnp.float32)
        blocks = kept + swap_bit(sent, axis, bit).astype(jnp.float32)
    return blocks[0]


def narrow(value):
    return lax.reduce_precision(value, 8, 7)


def split_terms(value, count):
    pieces = []
    for _ in range(count):
        piece = narrow(value)
        pieces.append(piece.astype(jnp.bfloat16))
        value = value - piece
    return pieces


def whole(*arrays):
    return [pl.BlockSpec(memory_space=pltpu.VMEM) for _ in arrays]


def norm_kernel(tokens_ref, gain_ref, out_ref):
    values = tokens_ref[...].astype(jnp.float32)
    scale = lax.rsqrt(jnp.mean(values * values, axis=1, keepdims=True) + EPS)
    normed = (values * scale * gain_ref[...]).astype(jnp.bfloat16)
    blocks, _, cols = out_ref.shape
    for block in range(blocks):
        out_ref[block] = normed[:, block * cols : (block + 1) * cols]


def normed_blocks(tokens, gain, blocks):
    rows, width = tokens.shape
    return pl.pallas_call(
        norm_kernel,
        out_shape=jax.ShapeDtypeStruct((blocks, rows, width // blocks), jnp.bfloat16),
        in_specs=whole(tokens, gain),
        out_specs=pl.BlockSpec(memory_space=pltpu.VMEM),
        name="first_norm",
    )(tokens, gain.reshape(1, width))


def attend_kernel(lengths_ref, query_ref, new_ref, forget_ref, cache_ref, gates_ref, out_ref):
    group, heads, lanes = query_ref.shape
    cache_len = cache_ref.shape[1]
    head_width = lanes // 2
    scale = head_width ** (-0.5)
    first = pl.program_id(0) * group
    position = lax.broadcasted_iota(jnp.int32, (heads, cache_len), 1)
    for item in range(group):
        length = lengths_ref[first + item]
        query = query_ref[item]
        cache = cache_ref[item]
        gates = gates_ref[item]
        last_gate = jnp.sum(jnp.where(position == length - 1, gates, 0.0), axis=1, keepdims=True)
        newest = last_gate + forget_ref[item]
        scores = lax.dot_general(
            query, cache, (((1,), (1,)), ((), ())), preferred_element_type=jnp.float32
        )
        scores = scores * scale + (newest - gates)
        scores = jnp.where(position < length, scores, -jnp.inf)
        fresh = new_ref[pl.ds(item, 1), :].astype(jnp.float32)
        own = jnp.sum(query.astype(jnp.float32) * fresh, axis=1, keepdims=True) * scale
        highest = jnp.maximum(jnp.max(scores, axis=1, keepdims=True), own)
        past_exp = jnp.exp(scores - highest)
        own_exp = jnp.exp(own - highest)
        total = jnp.sum(past_exp, axis=1, keepdims=True) + own_exp
        past = (past_exp / total).astype(jnp.bfloat16)
        own_share = (own_exp / total).astype(jnp.bfloat16).astype(jnp.float32)
        mixed = lax.dot_general(
            past, cache, (((1,), (0,)), ((), ())), preferred_element_type=jnp.float32
        )
        out_ref[item] = (mixed + own_share * fresh).astype(jnp.bfloat16)


def attend_fused(queries, key_new, value_new, forget, kv_cache, log_gates, lengths):
    seqs, cache_len, _, lanes = kv_cache.shape
    head_width = lanes // 2
    heads = queries.shape[1] // head_width
    wide = jnp.pad(queries.reshape(seqs, heads, head_width), ((0, 0), (0, 0), (0, head_width)))
    fresh = jnp.concatenate([key_new, value_new], axis=1)
    steps = 4 if seqs % 4 == 0 else 1
    group = seqs // steps
    out = pl.pallas_call(
        attend_kernel,
        out_shape=jax.ShapeDtypeStruct((seqs, heads, lanes), jnp.bfloat16),
        grid_spec=pltpu.PrefetchScalarGridSpec(
            num_scalar_prefetch=1,
            grid=(steps,),
            in_specs=[
                pl.BlockSpec((group, heads, lanes), lambda i, _: (i, 0, 0)),
                pl.BlockSpec((None, group, lanes), lambda i, _: (i, 0, 0)),
                pl.BlockSpec((group, heads, 1), lambda i, _: (i, 0, 0)),
                pl.BlockSpec((group, cache_len, lanes), lambda i, _: (i, 0, 0)),
                pl.BlockSpec((group, heads, cache_len), lambda i, _: (i, 0, 0)),
            ],
            out_specs=pl.BlockSpec((group, heads, lanes), lambda i, _: (i, 0, 0)),
        ),
        cost_estimate=pl.CostEstimate(
            flops=4 * seqs * heads * cache_len * lanes,
            transcendentals=seqs * heads * cache_len,
            bytes_accessed=seqs * cache_len * (2 * lanes + 4 * heads),
        ),
        name="attend",
    )(
        lengths,
        wide,
        fresh.reshape(steps, group, lanes),
        forget[:, :, None],
        kv_cache.reshape(seqs, cache_len, lanes),
        log_gates.transpose(0, 2, 1),
    )
    return out[:, :, head_width:].reshape(seqs, heads * head_width)


def silu(value):
    return value / (1.0 + jnp.exp(-value))


def load_all(pairs, sems):
    copies = [
        pltpu.make_async_copy(source, target, sems.at[i])
        for i, (source, target) in enumerate(pairs)
    ]
    for copy in copies:
        copy.start()
    return copies


def expert_kernel(
    index_ref,
    block0_ref,
    block1_ref,
    block2_ref,
    block3_ref,
    gain_ref,
    vector_ref,
    weight_ref,
    gate_hbm,
    up_hbm,
    down_hbm,
    send_ref,
    keep_ref,
    second_ref,
    value_ref,
    gate_ref,
    up_ref,
    down_ref,
    sems,
):
    index = index_ref[0]
    blocks = (block0_ref, block1_ref, block2_ref, block3_ref)
    sources, rows, cols = block0_ref.shape
    width, units = gate_ref.shape
    chunks = 4
    depth = width // chunks
    quarter = down_ref.shape[2]
    pairs = []
    for k in range(chunks):
        span = pl.ds(k * depth, depth)
        pairs.append((gate_hbm.at[span, :], gate_ref.at[span, :]))
        pairs.append((up_hbm.at[span, :], up_ref.at[span, :]))
    for j in range(4):
        start = pl.multiple_of((index ^ j) * quarter, quarter)
        pairs.append((down_hbm.at[:, pl.ds(start, quarter)], down_ref.at[j]))
    copies = load_all(pairs, sems)

    squares = jnp.zeros((rows, cols), jnp.float32)
    for j in range(4):
        for e in range(sources):
            values = blocks[j][e].astype(jnp.float32)
            squares = squares + values * values
    scale = lax.rsqrt(jnp.sum(squares, axis=1, keepdims=True) / width + EPS)
    logit = jnp.zeros((rows, cols), jnp.float32)
    for j in range(4):
        for e in range(sources):
            start = pl.multiple_of((e * 4 + (index ^ j)) * cols, cols)
            span = pl.ds(start, cols)
            values = blocks[j][e].astype(jnp.float32)
            second = (values * scale * gain_ref[:, span]).astype(jnp.bfloat16)
            second_ref[:, span] = second
            logit = logit + second.astype(jnp.float32) * vector_ref[:, span]
    value = 1.0 / (1.0 + jnp.exp(-jnp.sum(logit, axis=1, keepdims=True)))
    value_ref[...] = jnp.broadcast_to(value, value_ref.shape)

    gate = jnp.zeros((rows, units), jnp.float32)
    up = jnp.zeros((rows, units), jnp.float32)
    for k in range(chunks):
        span = slice(k * depth, (k + 1) * depth)
        left = second_ref[:, span]
        copies[2 * k].wait()
        gate = gate + jnp.dot(left, gate_ref[span, :], preferred_element_type=jnp.float32)
        copies[2 * k + 1].wait()
        up = up + jnp.dot(left, up_ref[span, :], preferred_element_type=jnp.float32)
    hidden = (silu(gate) * up).astype(jnp.bfloat16)
    weight = weight_ref[...]
    for j in (1, 3, 0, 2):
        copies[2 * chunks + j].wait()
        out = jnp.dot(hidden, down_ref[j], preferred_element_type=jnp.float32) * weight
        if j % 2:
            send_ref[j // 2] = out.astype(jnp.bfloat16)
        else:
            keep_ref[j // 2] = out


def expert_fused(index, blocks, gain, vector, weight, gate, up, down):
    sources, rows, cols = blocks[0].shape
    width, units = gate.shape
    quarter = width // 4
    hbm = pl.BlockSpec(memory_space=pltpu.HBM)
    vmem = pl.BlockSpec(memory_space=pltpu.VMEM)
    return pl.pallas_call(
        expert_kernel,
        out_shape=(
            jax.ShapeDtypeStruct((2, rows, quarter), jnp.bfloat16),
            jax.ShapeDtypeStruct((2, rows, quarter), jnp.float32),
            jax.ShapeDtypeStruct((rows, width), jnp.bfloat16),
            jax.ShapeDtypeStruct((rows, 128), jnp.float32),
        ),
        in_specs=[pl.BlockSpec(memory_space=pltpu.SMEM)] + [vmem] * 7 + [hbm] * 3,
        out_specs=[vmem] * 4,
        scratch_shapes=[
            pltpu.VMEM((width, units), jnp.bfloat16),
            pltpu.VMEM((width, units), jnp.bfloat16),
            pltpu.VMEM((4, units, quarter), jnp.bfloat16),
            pltpu.SemaphoreType.DMA((12,)),
        ],
        cost_estimate=pl.CostEstimate(
            flops=6 * rows * width * units, transcendentals=0, bytes_accessed=6 * width * units
        ),
        name="expert",
    )(
        index.reshape(1),
        *blocks,
        gain.reshape(1, width),
        vector.reshape(1, width),
        weight.reshape(rows, 1),
        gate,
        up,
        down,
    )


def dense_kernel(
    second_ref, value_ref, gate_hbm, up_hbm, down_hbm, out_ref, gate_ref, up_ref, down_ref, sems
):
    rows = second_ref.shape[0]
    width, units = gate_ref.shape
    chunks = 4
    depth = width // chunks
    pairs = []
    for k in range(chunks):
        span = pl.ds(k * depth, depth)
        pairs.append((gate_hbm.at[span, :], gate_ref.at[span, :]))
        pairs.append((up_hbm.at[span, :], up_ref.at[span, :]))
    pairs.append((down_hbm, down_ref))
    copies = load_all(pairs, sems)
    gate = jnp.zeros((rows, units), jnp.float32)
    up = jnp.zeros((rows, units), jnp.float32)
    for k in range(chunks):
        span = slice(k * depth, (k + 1) * depth)
        left = second_ref[:, span]
        copies[2 * k].wait()
        gate = gate + jnp.dot(left, gate_ref[span, :], preferred_element_type=jnp.float32)
        copies[2 * k + 1].wait()
        up = up + jnp.dot(left, up_ref[span, :], preferred_element_type=jnp.float32)
    hidden = (silu(gate) * up).astype(jnp.bfloat16)
    copies[2 * chunks].wait()
    out = jnp.dot(hidden, down_ref[...], preferred_element_type=jnp.float32)
    out_ref[...] = out * value_ref[:, :1]


def dense_fused(second, value, gate, up, down):
    rows, width = second.shape
    units = gate.shape[1]
    cols = down.shape[1]
    hbm = pl.BlockSpec(memory_space=pltpu.HBM)
    vmem = pl.BlockSpec(memory_space=pltpu.VMEM)
    return pl.pallas_call(
        dense_kernel,
        out_shape=jax.ShapeDtypeStruct((rows, cols), jnp.float32),
        in_specs=[vmem] * 2 + [hbm] * 3,
        out_specs=vmem,
        scratch_shapes=[
            pltpu.VMEM((width, units), jnp.bfloat16),
            pltpu.VMEM((width, units), jnp.bfloat16),
            pltpu.VMEM((units, cols), jnp.bfloat16),
            pltpu.SemaphoreType.DMA((9,)),
        ],
        cost_estimate=pl.CostEstimate(
            flops=2 * rows * units * (2 * width + cols),
            transcendentals=0,
            bytes_accessed=2 * units * (2 * width + cols),
        ),
        name="dense",
    )(second, value, gate, up, down)


def mix_by_columns(tokens, attended, out_weight):
    experts = lax.axis_size("ep")
    shares = lax.axis_size("tp")
    seq_count, width = tokens.shape
    rows = experts * seq_count
    block_cols = out_weight.shape[1] // shares
    own_tokens = lax.dynamic_index_in_dim(
        tokens.reshape(seq_count, experts, shares, block_cols),
        lax.axis_index("tp"),
        2,
        keepdims=False,
    ).transpose(1, 0, 2)
    sent = jnp.concatenate(
        [jnp.broadcast_to(attended, (experts,) + attended.shape), own_tokens], axis=2
    )
    got = lax.all_to_all(sent, "ep", split_axis=0, concat_axis=0, tiled=True)
    got = got.reshape(rows, -1)
    column_terms = jnp.dot(
        got[:, : attended.shape[1]], out_weight, preferred_element_type=jnp.float32
    )
    attention_out = keep_block(
        column_terms.reshape(rows, shares, block_cols).transpose(1, 0, 2), "tp"
    )
    mixed_block = (got[:, attended.shape[1] :].astype(jnp.float32) + attention_out).astype(
        jnp.bfloat16
    )
    gathered = lax.all_to_all(
        jnp.broadcast_to(mixed_block, (experts, rows, block_cols)),
        "ep",
        split_axis=0,
        concat_axis=0,
        tiled=True,
    )
    blocks = [gathered]
    for bit in bits_of("tp"):
        blocks = blocks + [None] * len(blocks)
    for bit in reversed(bits_of("tp")):
        for j, block in enumerate(list(blocks)):
            if block is not None and blocks[j ^ bit] is None:
                blocks[j ^ bit] = swap_bit(block, "tp", bit)
    return blocks


def own_residual(blocks, seq_count, quarter):
    index = lax.axis_index("tp")
    cols = blocks[0].shape[2]
    sources = quarter // (len(blocks) * cols)
    pieces = jnp.stack(
        [
            lax.dynamic_slice(
                block,
                (index * sources, lax.axis_index("ep") * seq_count, 0),
                (sources, seq_count, cols),
            )
            for block in blocks
        ]
    )
    order = jnp.arange(len(blocks), dtype=jnp.int32) ^ index
    return pieces[order].transpose(2, 1, 0, 3).reshape(seq_count, quarter)


def mix_by_rows(tokens, attended, out_weight):
    column_terms = jnp.dot(
        lax.all_gather(attended, "ep", axis=0, tiled=True),
        out_weight,
        preferred_element_type=jnp.float32,
    )
    summed = lax.all_to_all(
        lax.psum(column_terms, "tp"), "ep", split_axis=0, concat_axis=1, tiled=True
    )
    mixed = (tokens.astype(jnp.float32) + summed).astype(jnp.bfloat16)
    return lax.all_gather(mixed, "ep", axis=0, tiled=True)


def finish(residual, total):
    seq_count, quarter = residual.shape
    returned = lax.all_to_all(
        total.reshape(-1, seq_count, quarter), "ep", split_axis=0, concat_axis=0, tiled=True
    )
    return (
        residual.astype(jnp.float32) + jnp.sum(returned.astype(jnp.float32), axis=0)
    ).astype(jnp.bfloat16)


def shards(
    tokens,
    norm_gain,
    query_weight,
    key_weight,
    value_weight,
    forget_weight,
    forget_bias,
    kv_cache,
    log_gates,
    lengths,
    out_weight,
    mix_gain,
    expert_gate,
    expert_up,
    expert_down,
    routes,
    route_weights,
    dense_gate,
    dense_up,
    dense_down,
    gate_vector,
):
    experts = lax.axis_size("ep")
    shares = lax.axis_size("tp")
    ep_index = lax.axis_index("ep")
    tp_index = lax.axis_index("tp")
    seq_count, width = tokens.shape
    rows = experts * seq_count
    query_cols = query_weight.shape[1]
    key_cols = key_weight.shape[1]
    gate_cols = forget_weight.shape[1]

    normed = normed_blocks(tokens, norm_gain, experts)
    columns = lax.all_to_all(normed, "ep", split_axis=0, concat_axis=0, tiled=True)
    columns = columns.reshape(rows, width // experts)

    own_weight = jnp.sum(
        jnp.where(
            routes[None, :, :] == jnp.arange(experts, dtype=jnp.int32)[:, None, None],
            route_weights[None, :, :],
            0.0,
        ),
        axis=2,
    )
    split = query_cols + 2 * key_cols
    spare = -(split + 2 * gate_cols + 3) % 128
    weights = jnp.concatenate(
        [
            query_weight,
            key_weight,
            value_weight,
            forget_weight,
            forget_weight,
            jnp.zeros((query_weight.shape[0], 3 + spare), jnp.bfloat16),
        ],
        axis=1,
    )
    extra = jnp.pad(
        jnp.stack(split_terms(own_weight, 3), axis=2),
        ((0, 0), (0, 0), (split + 2 * gate_cols, spare)),
    ).reshape(rows, -1)
    terms = jnp.dot(columns, weights, preferred_element_type=jnp.float32)
    lane = lax.broadcasted_iota(jnp.int32, terms.shape, 1)
    second_term = (lane >= split + gate_cols) & (lane < split + 2 * gate_cols)
    sent = jnp.where(second_term, terms - narrow(terms), terms).astype(jnp.bfloat16)
    sent = jnp.where(lane < split + 2 * gate_cols, sent, extra)
    got = lax.all_to_all(
        sent.reshape(experts, seq_count, -1), "ep", split_axis=0, concat_axis=0, tiled=True
    )
    projected = jnp.sum(got[:, :, : split + 2 * gate_cols].astype(jnp.float32), axis=0)
    spot = split + 2 * gate_cols
    expert_weight = jnp.sum(got[:, :, spot : spot + 3].astype(jnp.float32), axis=2)
    queries = projected[:, :query_cols].astype(jnp.bfloat16)
    key_new = projected[:, query_cols : query_cols + key_cols].astype(jnp.bfloat16)
    value_new = projected[:, query_cols + key_cols : split].astype(jnp.bfloat16)
    forget = jax.nn.log_sigmoid(
        projected[:, split : split + gate_cols] + projected[:, split + gate_cols :] + forget_bias
    )
    if kv_cache.shape[2] == 1 and 2 * key_cols == 128:
        attended = attend_fused(
            queries, key_new, value_new, forget, kv_cache, log_gates, lengths
        )
    else:
        attended = attend_local(
            queries, key_new, value_new, forget, kv_cache, log_gates, lengths
        )

    capacity = max(2, 2 * seq_count * routes.shape[1] // experts)
    quarter = width // shares
    if out_weight.shape[1] == 128 * shares and shares == 4 and capacity >= seq_count:
        blocks = mix_by_columns(tokens, attended, out_weight)
        residual = own_residual(blocks, seq_count, quarter)
        send, keep, second, value = expert_fused(
            tp_index,
            blocks,
            mix_gain,
            gate_vector,
            expert_weight,
            expert_gate[0],
            expert_up[0],
            expert_down[0],
        )
        across = swap_bit(send, "tp", 1)
        far = swap_bit((keep[1] + across[1].astype(jnp.float32)).astype(jnp.bfloat16), "tp", 2)
        dense_terms = dense_fused(second, value, dense_gate, dense_up, dense_down)
        expert_sum = keep[0] + across[0].astype(jnp.float32) + far.astype(jnp.float32)
        total = (expert_sum + dense_terms).astype(jnp.bfloat16)
        return finish(residual, total)
    mixed = mix_by_rows(tokens, attended, out_weight)
    second = rms_scaled(mixed, mix_gain).astype(jnp.bfloat16)
    gate_value = jax.nn.sigmoid(jnp.sum(second.astype(jnp.float32) * gate_vector, axis=1))

    weight = expert_weight
    picked = second
    chooser = None
    if capacity < seq_count:
        taken = weight > 0
        place = jnp.cumsum(taken.astype(jnp.int32), axis=1) - 1
        chooser = (
            taken[:, None, :]
            & (place[:, None, :] == jnp.arange(capacity, dtype=jnp.int32)[None, :, None])
        ).astype(jnp.bfloat16)
        picked = jnp.einsum(
            "ecs,esd->ecd",
            chooser,
            second.reshape(experts, seq_count, width),
            preferred_element_type=jnp.float32,
        ).astype(jnp.bfloat16)
        picked = picked.reshape(experts * capacity, width)
        weight = jnp.einsum(
            "ecs,es->ec",
            chooser.astype(jnp.float32),
            weight,
            precision=lax.Precision.HIGHEST,
        )
    gate_pre = jnp.dot(picked, expert_gate[0], preferred_element_type=jnp.float32)
    up_pre = jnp.dot(picked, expert_up[0], preferred_element_type=jnp.float32)
    hidden = (jax.nn.silu(gate_pre) * up_pre).astype(jnp.bfloat16)
    expert_out = jnp.dot(hidden, expert_down[0], preferred_element_type=jnp.float32)
    expert_out = expert_out * weight.reshape(-1)[:, None]
    served = expert_out.shape[0]
    expert_sum = keep_block(
        expert_out.reshape(served, shares, quarter).transpose(1, 0, 2), "tp"
    )
    if chooser is not None:
        expert_sum = jnp.einsum(
            "ecs,ecd->esd",
            chooser,
            expert_sum.reshape(experts, capacity, quarter).astype(jnp.bfloat16),
            preferred_element_type=jnp.float32,
        ).reshape(rows, quarter)

    dense_hidden = (
        jax.nn.silu(jnp.dot(second, dense_gate, preferred_element_type=jnp.float32))
        * jnp.dot(second, dense_up, preferred_element_type=jnp.float32)
    ).astype(jnp.bfloat16)
    dense_terms = jnp.dot(dense_hidden, dense_down, preferred_element_type=jnp.float32)
    total = (expert_sum + gate_value[:, None] * dense_terms).astype(jnp.bfloat16)

    residual = lax.dynamic_slice(
        mixed, (ep_index * seq_count, tp_index * quarter), (seq_count, quarter)
    )
    return finish(residual, total)


def solution(mesh):
    return jax.shard_map(
        shards,
        mesh=mesh,
        in_specs=(
            P("ep", None),
            P(),
            P("ep", "tp"),
            P("ep", "tp"),
            P("ep", "tp"),
            P("ep", "tp"),
            P("tp"),
            P("ep", None, "tp", None),
            P("ep", None, "tp"),
            P("ep"),
            P("tp", "ep"),
            P(),
            P("ep", None, "tp"),
            P("ep", None, "tp"),
            P("ep", "tp", None),
            P("ep", None),
            P("ep", None),
            P(None, "ep"),
            P(None, "ep"),
            P("ep", "tp"),
            P(),
        ),
        out_specs=P("ep", "tp"),
        check_vma=False,
    )
```
